32 devices in a mesh: gr: 2 (over x), sp: 8 (over z, y), tp: 2 (over core).
Axes of the slice: x: 2, y: 2, z: 4, core: 2. Of those that a mesh axis runs over, the one named last changes fastest.
Arguments:
- tokens: bfloat16 [16, 512, 4096], P('gr', 'sp'), may hold values from -6 to 6
- key_weight: bfloat16 [4096, 2048], P(('gr', 'sp'), 'tp'), may hold values from -0.09375 to 0.09375
- value_weight: bfloat16 [4096, 2048], P(('gr', 'sp'), 'tp'), may hold values from -0.09375 to 0.09375
- gate_weight: bfloat16 [4096, 16], P(('gr', 'sp'), 'tp'), may hold values from -0.09375 to 0.09375
- forget_bias: float32 [16], P('tp'), may hold values from 7 to 9
- new_query: bfloat16 [16, 16, 128], P('gr', 'tp'), may hold values from -6 to 6
Outputs:
- key_cache: bfloat16 [16, 16, 512, 128], P(('gr', 'sp'), 'tp')
- value_cache: bfloat16 [16, 16, 512, 128], P(('gr', 'sp'), 'tp')
- gate_cache: float32 [16, 16, 512], P(('gr', 'sp'), 'tp')
- first_read: bfloat16 [16, 16, 128], P(('gr', 'sp'), 'tp')
The draws below stay inside these ranges and needn't reach their ends.
All inputs are finite; a program needn't handle non-finite values.
Results may differ from the reference program's by a relative error of at most 0.0075.
Values may be sent and summed in bfloat16 or wider, within the bound.
A program may use at most 64 MiB of HBM per device.

```python
import jax
import jax.numpy as jnp
from jax import lax

D = 4096
HEADS = 16
HEAD_DIM = 128
PROMPT = 512
SEQUENCES = 16


def shard_levels(key, dims, split, low, top_value):
    factor_of, own = 1.0, jax.random.fold_in(key, 6)
    for axis_at, blocks in split:
        heights = jnp.exp(jax.random.uniform(jax.random.fold_in(own, axis_at), (blocks,), jnp.float32, low / len(split), top_value / len(split)))
        factor_of = factor_of * jnp.repeat(heights, dims[axis_at] // blocks).reshape([-1 if axis == axis_at else 1 for axis in range(len(dims))])
    return factor_of


def centred(key, dims, scale, bound, split=(), held_as=jnp.bfloat16):
    values = scale * jax.random.normal(key, dims, jnp.float32)
    if split:
        values = values * shard_levels(key, dims, split, -0.22, 0.18)
    return jnp.clip(values, -bound, bound).astype(held_as)


def setup_inputs(seed: int = 0) -> dict:
    streams_of = jax.random.split(jax.random.key(seed), 7)
    tokens = centred(streams_of[0], (SEQUENCES, PROMPT, D), 1.0, 6.0, ((0, 2), (1, 8)))
    key_weight = centred(streams_of[1], (D, HEADS * HEAD_DIM), D ** -0.5, 0.09375, ((0, 16), (1, 2)))
    value_weight = centred(streams_of[2], (D, HEADS * HEAD_DIM), D ** -0.5, 0.09375, ((0, 16), (1, 2)))
    gate_weight = centred(streams_of[3], (D, HEADS), D ** -0.5, 0.09375, ((0, 16), (1, 2)))
    forget_bias = jnp.clip(7.0 + 2.0 * jax.random.uniform(streams_of[4], (HEADS,), jnp.float32) ** shard_levels(streams_of[4], (HEADS,), ((0, 2),), -0.2, 0.2), 7.0, 9.0)
    new_query = centred(streams_of[5], (SEQUENCES, HEADS, HEAD_DIM), 1.0, 6.0, ((0, 2), (1, 2)))
    return {"tokens": tokens, "key_weight": key_weight, "value_weight": value_weight, "gate_weight": gate_weight, "forget_bias": forget_bias, "new_query": new_query}


eps = 1e-06

def reference(tokens, key_weight, value_weight, gate_weight, forget_bias, new_query):
    scaling = HEAD_DIM ** (-0.5)

    def one_sequence(operands):
        rows, query = operands
        keys = jnp.dot(rows, key_weight, preferred_element_type=jnp.float32).astype(jnp.bfloat16)
        values = jnp.dot(rows, value_weight, preferred_element_type=jnp.float32).astype(jnp.bfloat16)
        logits = jnp.dot(rows, gate_weight, preferred_element_type=jnp.float32)
        keys = keys.reshape(PROMPT, HEADS, HEAD_DIM).transpose(1, 0, 2)
        values = values.reshape(PROMPT, HEADS, HEAD_DIM).transpose(1, 0, 2)
        log_gate = jax.nn.log_sigmoid(logits + forget_bias[None, :])
        cumulative = jnp.cumsum(log_gate, axis=0).T
        scores = jnp.einsum('hd,hsd->hs', query.astype(jnp.float32), keys.astype(jnp.float32)) * scaling
        scores = scores + cumulative[:, -1:] - cumulative
        probs = jax.nn.softmax(scores, axis=-1)
        attended = jnp.einsum('hs,hsd->hd', probs, values.astype(jnp.float32))
        normed = attended * lax.rsqrt(lax.optimization_barrier(jnp.mean(attended * attended, axis=-1, keepdims=True)) + eps)
        return (keys, values, cumulative, normed.astype(jnp.bfloat16))
    key_cache, value_cache, gate_cache, first_read = lax.map(one_sequence, (tokens, new_query))
    return (key_cache, value_cache, gate_cache, first_read)
```

```python
import functools

import jax
import jax.numpy as jnp
from jax import lax
from jax.experimental import pallas as pl
from jax.experimental.pallas import tpu as pltpu
from jax.sharding import PartitionSpec as P

eps = 1e-06
MESH = pl.DeviceIdType.MESH


def exchange(
    gr_size, sp_size, tokens, weights, gate_rows, kv_out, gate_out,
    tok, full, gates, staged, gate_staged,
    tok_send, tok_recv, mate_send, mate_recv, w_send, w_recv, z_send, z_recv,
    gw_send, gw_recv, g_send, g_recv, o_send, o_recv, local,
):
    g, s, t = lax.axis_index("gr"), lax.axis_index("sp"), lax.axis_index("tp")
    y, z = lax.rem(s, 2), s // 2
    levels = sp_size // 2
    sequences, positions, features = tokens.shape
    depth, width = weights.shape[1], full.shape[1]
    head_dim = kv_out.shape[2]
    heads = width // head_dim
    members = gr_size * sp_size
    me = g * sp_size + s
    mate = t + 1 - 2 * lax.rem(t, 2)
    core = lax.rem(t, 2)
    quarter = sequences // 4

    gr_of = (g, 1 - g, g, 1 - g)
    y_of = (y, y, 1 - y, 1 - y)

    def where(r, level=None):
        return (gr_of[r], (z if level is None else level) * 2 + y_of[r], t)

    def remote(src, dst, send, recv, device):
        return pltpu.make_async_remote_copy(
            src_ref=src, dst_ref=dst, send_sem=send, recv_sem=recv,
            device_id=device, device_id_type=MESH,
        )

    barrier = pltpu.get_barrier_semaphore()

    def greet(k, carry):
        @pl.when(k != me)
        def _():
            pl.semaphore_signal(
                barrier, inc=1, device_id=(k // sp_size, lax.rem(k, sp_size), t),
                device_id_type=MESH,
            )
        return carry

    lax.fori_loop(0, members, greet, 0)
    pl.semaphore_signal(barrier, inc=1, device_id=(g, s, mate), device_id_type=MESH)
    pl.semaphore_wait(barrier, members)

    def rows_at(r, level):
        return full.at[pl.ds(pl.multiple_of((gr_of[r] * sp_size + level * 2 + y_of[r]) * depth, depth), depth), :]

    def part_for(r):
        return weights.at[gr_of[r], :, pl.ds(pl.multiple_of(y_of[r] * width, width), width)]

    def w_copy(r):
        return remote(part_for(r), rows_at(0, z), w_send.at[r], w_recv.at[r], where(r))

    def w_landing(r):
        return remote(part_for(r), rows_at(r, z), w_send.at[r], w_recv.at[r], where(r))

    def z_copy(direction, r, level, src=None):
        block = rows_at(r, level)
        to = z + 1 if direction == 0 else z - 1
        return remote(
            block if src is None else src, block, z_send.at[direction, level, r],
            z_recv.at[level, r], where(0, to),
        )

    def can_send(direction):
        return z < levels - 1 if direction == 0 else z > 0

    def pass_on(direction, r, level, src=None):
        @pl.when(can_send(direction))
        def _():
            z_copy(direction, r, level, src).start()

    own_part = part_for(0)
    for r in (3, 1, 2):
        w_copy(r).start()
    for direction in range(2):
        pass_on(direction, 0, z, own_part)
    own_rows = pltpu.make_async_copy(own_part, rows_at(0, z), local.at[0])
    own_rows.start()
    own_tokens = pltpu.make_async_copy(tokens, tok.at[0], local.at[1])
    own_tokens.start()

    def gw_copy(k):
        return remote(
            gate_rows, gates.at[me], gw_send.at[k], gw_recv.at[me],
            (k // sp_size, lax.rem(k, sp_size), t),
        )

    def gw_landing(k):
        return remote(
            gate_rows, gates.at[k], gw_send.at[k], gw_recv.at[k],
            (k // sp_size, lax.rem(k, sp_size), t),
        )

    def others(fn):
        def turn(k, carry):
            @pl.when(k != me)
            def _():
                fn(k)
            return carry
        lax.fori_loop(0, members, turn, 0)

    others(lambda k: gw_copy(k).start())
    own_gate = pltpu.make_async_copy(gate_rows, gates.at[me], local.at[2])
    own_gate.start()

    def piece(ref, half, c):
        return ref.at[pl.ds((half * 2 + c) * quarter, quarter)]

    def tok_copy(r, c):
        return remote(
            piece(tokens, core, c), piece(tok.at[r], core, c),
            tok_send.at[r, c], tok_recv.at[r, c], where(r),
        )

    def corner_copy(via, c):
        return remote(
            piece(tok.at[via], core, c), piece(tok.at[3], core, c),
            tok_send.at[3, c], tok_recv.at[3, c], where(3 - via),
        )

    def mate_copy(r, c, half):
        return remote(
            piece(tok.at[r], half, c), piece(tok.at[r], half, c),
            mate_send.at[r, c], mate_recv.at[r, c], (g, s, mate),
        )

    for c in range(2):
        tok_copy(1, c).start()
        tok_copy(2, 1 - c).start()

    def token_arrival(r, c):
        tok_copy(r, c).wait_recv()
        mate_copy(r, c, core).start()

    own_gate.wait()
    own_tokens.wait()
    for r in (1, 2, 3):
        w_landing(r).wait_recv()
        for direction in range(2):
            pass_on(direction, r, z)

    others(lambda k: gw_landing(k).wait_recv())
    gate_full = jnp.concatenate([gates[k] for k in range(members)], axis=1).astype(jnp.bfloat16)

    def gate_copy(k):
        return remote(
            gate_staged.at[k], gate_out.at[s], g_send.at[k], g_recv.at[s], (g, k, t)
        )

    def gate_landing(k):
        return remote(
            gate_staged.at[k], gate_out.at[k], g_send.at[k], g_recv.at[k], (g, k, t)
        )

    def gate_turn(k, carry):
        gate_staged[k] = lax.dot_general(
            gate_full, tok[0, k], (((1,), (1,)), ((), ())),
            preferred_element_type=jnp.float32,
        )
        @pl.when(k != s)
        def _():
            gate_copy(k).start()
        @pl.when(k == s)
        def _():
            pltpu.make_async_copy(gate_staged.at[k], gate_out.at[k], local.at[3]).start()
        return carry

    lax.fori_loop(0, sequences, gate_turn, 0)

    def z_step(j):
        for r in range(4):
            @pl.when(z - j >= 0)
            def _():
                z_copy(0, r, z - j).wait_recv()
                pass_on(0, r, z - j)
            @pl.when(z + j < levels)
            def _():
                z_copy(1, r, z + j).wait_recv()
                pass_on(1, r, z + j)

    z_step(1)
    token_arrival(1, 0)
    corner_copy(1, 0).start()
    token_arrival(2, 1)
    corner_copy(2, 1).start()
    for j in range(2, levels - 1):
        z_step(j)
    token_arrival(1, 1)
    token_arrival(2, 0)
    if levels > 2:
        z_step(levels - 1)
    own_rows.wait()

    tile = min(width, 2 * head_dim)
    tiles = width // tile
    group = min(sequences, max(1, 512 // positions))
    groups = sequences // group

    def out_copy(r, k):
        return remote(
            staged.at[r, :, k],
            kv_out.at[pl.ds((g * 2 + y) * heads, heads), pl.ds(pl.multiple_of((z * 2 + y_of[r]) * positions, positions), positions), :],
            o_send.at[r, k], o_recv.at[me, y_of[r]], (gr_of[r], k, t),
        )

    def out_landing(k, b):
        their_g, their_s = k // sp_size, lax.rem(k, sp_size)
        their_y, their_z = lax.rem(their_s, 2), their_s // 2
        return remote(
            staged.at[0, :, 0],
            kv_out.at[pl.ds((their_g * 2 + their_y) * heads, heads), pl.ds(pl.multiple_of((their_z * 2 + b) * positions, positions), positions), :],
            o_send.at[0, 0], o_recv.at[k, b], (their_g, their_s, t),
        )

    def keep_copy(r):
        return pltpu.make_async_copy(
            staged.at[r, :, s],
            kv_out.at[pl.ds((g * 2 + y) * heads, heads), pl.ds(pl.multiple_of((z * 2 + y_of[r]) * positions, positions), positions), :],
            local.at[4 + r],
        )

    def products(r):
        def turn(i, carry):
            m, n = i // tiles, lax.rem(i, tiles)
            rows = tok[r, pl.ds(m * group, group)].reshape(group * positions, features)
            columns = full[:, pl.ds(pl.multiple_of(n * tile, tile), tile)]
            out = jnp.dot(rows, columns, preferred_element_type=jnp.float32).astype(jnp.bfloat16)
            for h in range(tile // head_dim):
                staged[r, n * (tile // head_dim) + h, pl.ds(m * group, group)] = out[
                    :, h * head_dim : (h + 1) * head_dim
                ].reshape(group, positions, head_dim)
            return carry

        lax.fori_loop(0, groups * tiles, turn, 0)

        def send(i, carry):
            k = lax.rem(s + 1 + i, sp_size)
            if r in (1, 3):
                out_copy(r, k).start()
            else:
                @pl.when(k != s)
                def _():
                    out_copy(r, k).start()
                @pl.when(k == s)
                def _():
                    keep_copy(r).start()
            return carry

        lax.fori_loop(0, sequences, send, 0)

    products(0)
    for r in (1, 2):
        for c in range(2):
            mate_copy(r, c, 1 - core).wait_recv()
        products(r)
    for c in range(2):
        token_arrival(3, c)
    for c in range(2):
        mate_copy(3, c, 1 - core).wait_recv()
    products(3)

    def landed(k):
        for b in range(2):
            out_landing(k, b).wait_recv()

    others(landed)
    keep_copy(0).wait()
    keep_copy(2).wait()

    def gate_landed(k, carry):
        @pl.when(k != s)
        def _():
            gate_landing(k).wait_recv()
            gate_copy(k).wait_send()
        @pl.when(k == s)
        def _():
            pltpu.make_async_copy(gate_staged.at[k], gate_out.at[k], local.at[3]).wait()
        return carry

    lax.fori_loop(0, sequences, gate_landed, 0)
    others(lambda k: gw_copy(k).wait_send())
    for r in (1, 2, 3):
        w_copy(r).wait_send()
        for c in range(2):
            mate_copy(r, c, core).wait_send()
    for c in range(2):
        tok_copy(1, c).wait_send()
        tok_copy(2, c).wait_send()
    corner_copy(1, 0).wait_send()
    corner_copy(2, 1).wait_send()
    for r in range(4):
        def sent(k, carry):
            if r in (1, 3):
                out_copy(r, k).wait_send()
            else:
                @pl.when(k != s)
                def _():
                    out_copy(r, k).wait_send()
            return carry
        lax.fori_loop(0, sequences, sent, 0)
    for r in range(4):
        for direction in range(2):
            @pl.when(can_send(direction))
            def _():
                z_copy(direction, r, z, own_part if r == 0 else None).wait_send()
        for j in range(1, levels):
            @pl.when((z - j >= 0) & can_send(0))
            def _():
                z_copy(0, r, z - j).wait_send()
            @pl.when((z + j < levels) & can_send(1))
            def _():
                z_copy(1, r, z + j).wait_send()


def on_device(gr_size, sp_size, tokens, key_weight, value_weight, gate_weight, forget_bias, new_query):
    sequences, positions, features = tokens.shape
    heads_here = forget_bias.shape[0]
    head_dim = new_query.shape[2]
    scaling = head_dim ** (-0.5)
    members = gr_size * sp_size
    depth = key_weight.shape[0]
    width = 2 * key_weight.shape[1] // 4
    weights = jnp.stack([key_weight, value_weight])
    gate_rows = gate_weight.T.astype(jnp.float32)
    levels = sp_size // 2
    dma = pltpu.SemaphoreType.DMA
    kv, logits = pl.pallas_call(
        functools.partial(exchange, gr_size, sp_size),
        out_shape=(
            jax.ShapeDtypeStruct((2 * heads_here, sp_size * positions, head_dim), jnp.bfloat16),
            jax.ShapeDtypeStruct((sp_size, heads_here, positions), jnp.float32),
        ),
        in_specs=[pl.BlockSpec(memory_space=pl.ANY)] * 3,
        out_specs=(pl.BlockSpec(memory_space=pl.ANY),) * 2,
        scratch_shapes=[
            pltpu.VMEM((4, sequences, positions, features), jnp.bfloat16),
            pltpu.VMEM((features, width), jnp.bfloat16),
            pltpu.VMEM((members, heads_here, depth), jnp.float32),
            pltpu.VMEM((4, width // head_dim, sequences, positions, head_dim), jnp.bfloat16),
            pltpu.VMEM((sequences, heads_here, positions), jnp.float32),
            dma((4, 2)), dma((4, 2)), dma((4, 2)), dma((4, 2)),
            dma((4,)), dma((4,)),
            dma((2, levels, 4)), dma((levels, 4)),
            dma((members,)), dma((members,)),
            dma((sp_size,)), dma((sp_size,)),
            dma((4, sp_size)), dma((members, 2)),
            dma((8,)),
        ],
        compiler_params=pltpu.CompilerParams(
            collective_id=0, has_side_effects=True, vmem_limit_bytes=60 * 1024 * 1024
        ),
    )(tokens, weights, gate_rows)
    key_cache, value_cache = kv[:heads_here], kv[heads_here:]
    logit = logits.transpose(1, 0, 2).reshape(heads_here, sp_size * positions)
    log_gate = jax.nn.log_sigmoid(logit + forget_bias[:, None])
    cumulative = jnp.cumsum(log_gate, axis=1)
    query = lax.dynamic_index_in_dim(new_query, lax.axis_index("sp"), 0, keepdims=False)
    scores = (
        jnp.einsum("hd,hpd->hp", query, key_cache, preferred_element_type=jnp.float32) * scaling
        + cumulative[:, -1:] - cumulative
    )
    highest = jnp.max(scores, axis=1, keepdims=True)
    probs = jnp.exp(scores - highest)
    total = jnp.sum(probs, axis=1)
    attended = jnp.einsum("hp,hpd->hd", probs, value_cache.astype(jnp.float32)) / total[:, None]
    normed = attended * lax.rsqrt(jnp.mean(attended * attended, axis=-1, keepdims=True) + eps)
    return (
        key_cache[None], value_cache[None], cumulative[None], normed.astype(jnp.bfloat16)[None]
    )


def solution(mesh):
    in_specs = (
        P("gr", "sp", None),
        P(("gr", "sp"), "tp"),
        P(("gr", "sp"), "tp"),
        P(("gr", "sp"), "tp"),
        P("tp"),
        P("gr", "tp", None),
    )
    out_specs = (
        P(("gr", "sp"), "tp", None, None),
        P(("gr", "sp"), "tp", None, None),
        P(("gr", "sp"), "tp", None),
        P(("gr", "sp"), "tp", None),
    )
    return jax.shard_map(
        functools.partial(on_device, mesh.shape["gr"], mesh.shape["sp"]),
        mesh=mesh, in_specs=in_specs, out_specs=out_specs, check_vma=False,
    )
```

```python
import functools

import jax
import jax.numpy as jnp
from jax import lax
from jax.experimental import pallas as pl
from jax.experimental.pallas import tpu as pltpu
from jax.sharding import PartitionSpec as P

eps = 1e-06
MESH = pl.DeviceIdType.MESH


def exchange(
    gr_size, sp_size, tokens, key_weight, value_weight, gate_rows, kv_out, gate_out,
    tok, weights, full, gates, staged, gate_staged,
    tok_send, tok_recv, mate_send, mate_recv, w_send, w_recv, z_send, z_recv,
    gw_send, gw_recv, g_send, g_recv, o_send, o_recv, kept, local,
):
    g, s, t = lax.axis_index("gr"), lax.axis_index("sp"), lax.axis_index("tp")
    y, z = lax.rem(s, 2), s // 2
    levels = sp_size // 2
    sequences, positions, features = tokens.shape
    depth = weights.shape[1]
    parts, tile = full.shape[0], full.shape[2]
    width = parts * tile
    head_dim = kv_out.shape[2]
    heads = width // head_dim
    tile_heads = tile // head_dim
    members = gr_size * sp_size
    me = g * sp_size + s
    mate = t + 1 - 2 * lax.rem(t, 2)
    core = lax.rem(t, 2)
    quarter = sequences // 4

    gr_of = (g, 1 - g, g, 1 - g)
    y_of = (y, y, 1 - y, 1 - y)

    def where(r, level=None):
        return (gr_of[r], (z if level is None else level) * 2 + y_of[r], t)

    def remote(src, dst, send, recv, device):
        return pltpu.make_async_remote_copy(
            src_ref=src, dst_ref=dst, send_sem=send, recv_sem=recv,
            device_id=device, device_id_type=MESH,
        )

    taken = [
        pltpu.make_async_copy(ref, weights.at[k], local.at[k])
        for k, ref in enumerate((key_weight, value_weight))
    ]
    for copy in taken:
        copy.start()
    own_tokens = pltpu.make_async_copy(tokens, tok.at[0], local.at[2])
    own_tokens.start()
    own_gate = pltpu.make_async_copy(gate_rows, gates.at[me], local.at[3])
    own_gate.start()
    barrier = pltpu.get_barrier_semaphore()

    def greet(k, carry):
        @pl.when(k != me)
        def _():
            pl.semaphore_signal(
                barrier, inc=1, device_id=(k // sp_size, lax.rem(k, sp_size), t),
                device_id_type=MESH,
            )
        return carry

    lax.fori_loop(0, members, greet, 0)
    pl.semaphore_signal(barrier, inc=1, device_id=(g, s, mate), device_id_type=MESH)
    pl.semaphore_wait(barrier, members)

    def rows_at(r, level, c):
        return full.at[c, pl.ds(pl.multiple_of((gr_of[r] * sp_size + level * 2 + y_of[r]) * depth, depth), depth), :]

    def part_for(r, c):
        return weights.at[gr_of[r], :, pl.ds(pl.multiple_of(y_of[r] * width + c * tile, tile), tile)]

    def w_copy(r, c):
        return remote(part_for(r, c), rows_at(0, z, c), w_send.at[r, c], w_recv.at[r, c], where(r))

    def w_landing(r, c):
        return remote(part_for(r, c), rows_at(r, z, c), w_send.at[r, c], w_recv.at[r, c], where(r))

    def z_copy(direction, r, level, c, src=None):
        block = rows_at(r, level, c)
        to = z + 1 if direction == 0 else z - 1
        return remote(
            block if src is None else src, block, z_send.at[direction, level, r, c],
            z_recv.at[level, r, c], where(0, to),
        )

    def can_send(direction):
        return z < levels - 1 if direction == 0 else z > 0

    def pass_on(direction, r, level, c, src=None):
        @pl.when(can_send(direction))
        def _():
            z_copy(direction, r, level, c, src).start()

    def level_out(c):
        for direction in range(2):
            pass_on(direction, 0, z, c, part_for(0, c))
        for r in (1, 2, 3):
            w_landing(r, c).wait_recv()
            for direction in range(2):
                pass_on(direction, r, z, c)

    for copy in taken:
        copy.wait()
    for c in range(parts):
        for r in (3, 1, 2):
            w_copy(r, c).start()

    def gw_copy(k):
        return remote(
            gate_rows, gates.at[me], gw_send.at[k], gw_recv.at[me],
            (k // sp_size, lax.rem(k, sp_size), t),
        )

    def gw_landing(k):
        return remote(
            gate_rows, gates.at[k], gw_send.at[k], gw_recv.at[k],
            (k // sp_size, lax.rem(k, sp_size), t),
        )

    def others(fn):
        def turn(k, carry):
            @pl.when(k != me)
            def _():
                fn(k)
            return carry
        lax.fori_loop(0, members, turn, 0)

    others(lambda k: gw_copy(k).start())
    def piece(ref, half, c):
        return ref.at[pl.ds((half * 2 + c) * quarter, quarter)]

    def tok_copy(r, c):
        return remote(
            piece(tokens, core, c), piece(tok.at[r], core, c),
            tok_send.at[r, c], tok_recv.at[r, c], where(r),
        )

    def corner_copy(via, c):
        return remote(
            piece(tok.at[via], core, c), piece(tok.at[3], core, c),
            tok_send.at[3, c], tok_recv.at[3, c], where(3 - via),
        )

    def mate_copy(r, c, half):
        return remote(
            piece(tok.at[r], half, c), piece(tok.at[r], half, c),
            mate_send.at[r, c], mate_recv.at[r, c], (g, s, mate),
        )

    for c in range(2):
        tok_copy(1, c).start()
        tok_copy(2, 1 - c).start()

    def token_arrival(r, c):
        tok_copy(r, c).wait_recv()
        mate_copy(r, c, core).start()

    level_out(0)
    own_gate.wait()
    own_tokens.wait()

    others(lambda k: gw_landing(k).wait_recv())
    gate_full = jnp.concatenate([gates[k] for k in range(members)], axis=1).astype(jnp.bfloat16)

    def gate_copy(k):
        return remote(
            gate_staged.at[k], gate_out.at[s], g_send.at[k], g_recv.at[s], (g, k, t)
        )

    def gate_landing(k):
        return remote(
            gate_staged.at[k], gate_out.at[k], g_send.at[k], g_recv.at[k], (g, k, t)
        )

    def gate_turn(k, carry):
        gate_staged[k] = lax.dot_general(
            gate_full, tok[0, k], (((1,), (1,)), ((), ())),
            preferred_element_type=jnp.float32,
        )
        @pl.when(k != s)
        def _():
            gate_copy(k).start()
        @pl.when(k == s)
        def _():
            pltpu.make_async_copy(gate_staged.at[k], gate_out.at[k], local.at[4]).start()
        return carry

    lax.fori_loop(0, sequences, gate_turn, 0)

    def z_step(j, c):
        for r in range(4):
            @pl.when(z - j >= 0)
            def _():
                z_copy(0, r, z - j, c).wait_recv()
                pass_on(0, r, z - j, c)
            @pl.when(z + j < levels)
            def _():
                z_copy(1, r, z + j, c).wait_recv()
                pass_on(1, r, z + j, c)

    group = min(sequences, max(1, 512 // positions))
    groups = sequences // group

    def cache_at(their_g, their_y, their_z, b, c):
        return kv_out.at[
            pl.ds((their_g * 2 + their_y) * heads + c * tile_heads, tile_heads),
            pl.ds(pl.multiple_of((their_z * 2 + b) * positions, positions), positions),
            :,
        ]

    def out_copy(r, k, c):
        return remote(
            staged.at[r, c, :, k], cache_at(g, y, z, y_of[r], c),
            o_send.at[r, k, c], o_recv.at[me, y_of[r], c], (gr_of[r], k, t),
        )

    def out_landing(k, b, c):
        their_g, their_s = k // sp_size, lax.rem(k, sp_size)
        their_y, their_z = lax.rem(their_s, 2), their_s // 2
        return remote(
            staged.at[0, c, :, 0], cache_at(their_g, their_y, their_z, b, c),
            o_send.at[0, 0, c], o_recv.at[k, b, c], (their_g, their_s, t),
        )

    def keep_copy(r, c):
        return pltpu.make_async_copy(
            staged.at[r, c, :, s], cache_at(g, y, z, y_of[r], c), kept.at[r, c]
        )

    def products(r, c):
        def turn(m, carry):
            rows = tok[r, pl.ds(m * group, group)].reshape(group * positions, features)
            out = jnp.dot(rows, full[c], preferred_element_type=jnp.float32).astype(jnp.bfloat16)
            for h in range(tile_heads):
                staged[r, c, h, pl.ds(m * group, group)] = out[
                    :, h * head_dim : (h + 1) * head_dim
                ].reshape(group, positions, head_dim)
            return carry

        lax.fori_loop(0, groups, turn, 0)

        def send(i, carry):
            k = lax.rem(s + 1 + i, sp_size)
            if r in (1, 3):
                out_copy(r, k, c).start()
            else:
                @pl.when(k != s)
                def _():
                    out_copy(r, k, c).start()
                @pl.when(k == s)
                def _():
                    keep_copy(r, c).start()
            return carry

        lax.fori_loop(0, sequences, send, 0)

    def keep_rows(c):
        at = pl.multiple_of(me * depth, depth)
        columns = pl.ds(pl.multiple_of(y * width + c * tile, tile), tile)
        full[c, pl.ds(at, depth), :] = weights[g, :, columns]

    for c in range(parts):
        keep_rows(c)
    last = levels - 1
    for j in range(1, last):
        z_step(j, 0)
    for c in range(1, parts):
        level_out(c)
    token_arrival(1, 0)
    corner_copy(1, 0).start()
    token_arrival(2, 1)
    corner_copy(2, 1).start()
    z_step(last, 0)
    products(0, 0)
    for c in range(1, parts):
        z_step(1, c) if last > 1 else None
    token_arrival(1, 1)
    token_arrival(2, 0)
    for c in range(1, parts):
        for j in range(2, last):
            z_step(j, c)
    for r in (1, 2):
        for c in range(2):
            mate_copy(r, c, 1 - core).wait_recv()
        products(r, 0)
    for c in range(1, parts):
        z_step(last, c)
        for r in (0, 1, 2):
            products(r, c)
    for c in range(2):
        token_arrival(3, c)
    for c in range(2):
        mate_copy(3, c, 1 - core).wait_recv()
    for c in range(parts):
        products(3, c)

    def landed(k):
        for b in range(2):
            for c in range(parts):
                out_landing(k, b, c).wait_recv()

    others(landed)
    for c in range(parts):
        keep_copy(0, c).wait()
        keep_copy(2, c).wait()

    def gate_landed(k, carry):
        @pl.when(k != s)
        def _():
            gate_landing(k).wait_recv()
            gate_copy(k).wait_send()
        @pl.when(k == s)
        def _():
            pltpu.make_async_copy(gate_staged.at[k], gate_out.at[k], local.at[4]).wait()
        return carry

    lax.fori_loop(0, sequences, gate_landed, 0)
    others(lambda k: gw_copy(k).wait_send())
    for r in (1, 2, 3):
        for c in range(parts):
            w_copy(r, c).wait_send()
        for c in range(2):
            mate_copy(r, c, core).wait_send()
    for c in range(2):
        tok_copy(1, c).wait_send()
        tok_copy(2, c).wait_send()
    corner_copy(1, 0).wait_send()
    corner_copy(2, 1).wait_send()
    for r in range(4):
        def sent(k, carry):
            for c in range(parts):
                if r in (1, 3):
                    out_copy(r, k, c).wait_send()
                else:
                    @pl.when(k != s)
                    def _():
                        out_copy(r, k, c).wait_send()
            return carry
        lax.fori_loop(0, sequences, sent, 0)
    for r in range(4):
        for c in range(parts):
            for direction in range(2):
                @pl.when(can_send(direction))
                def _():
                    z_copy(direction, r, z, c, part_for(0, c) if r == 0 else None).wait_send()
            for j in range(1, levels):
                @pl.when((z - j >= 0) & can_send(0))
                def _():
                    z_copy(0, r, z - j, c).wait_send()
                @pl.when((z + j < levels) & can_send(1))
                def _():
                    z_copy(1, r, z + j, c).wait_send()


def on_device(gr_size, sp_size, tokens, key_weight, value_weight, gate_weight, forget_bias, new_query):
    sequences, positions, features = tokens.shape
    heads_here = forget_bias.shape[0]
    head_dim = new_query.shape[2]
    scaling = head_dim ** (-0.5)
    members = gr_size * sp_size
    depth = key_weight.shape[0]
    width = 2 * key_weight.shape[1] // 4
    parts = 2 if width >= 2 * head_dim else 1
    tile = width // parts
    gate_rows = gate_weight.T.astype(jnp.float32)
    levels = sp_size // 2
    dma = pltpu.SemaphoreType.DMA
    kv, logits = pl.pallas_call(
        functools.partial(exchange, gr_size, sp_size),
        out_shape=(
            jax.ShapeDtypeStruct((2 * heads_here, sp_size * positions, head_dim), jnp.bfloat16),
            jax.ShapeDtypeStruct((sp_size, heads_here, positions), jnp.float32),
        ),
        in_specs=[pl.BlockSpec(memory_space=pl.ANY)] * 4,
        out_specs=(pl.BlockSpec(memory_space=pl.ANY),) * 2,
        scratch_shapes=[
            pltpu.VMEM((4, sequences, positions, features), jnp.bfloat16),
            pltpu.VMEM((2, depth, key_weight.shape[1]), jnp.bfloat16),
            pltpu.VMEM((parts, features, tile), jnp.bfloat16),
            pltpu.VMEM((members, heads_here, depth), jnp.float32),
            pltpu.VMEM((4, parts, tile // head_dim, sequences, positions, head_dim), jnp.bfloat16),
            pltpu.VMEM((sequences, heads_here, positions), jnp.float32),
            dma((4, 2)), dma((4, 2)), dma((4, 2)), dma((4, 2)),
            dma((4, parts)), dma((4, parts)),
            dma((2, levels, 4, parts)), dma((levels, 4, parts)),
            dma((members,)), dma((members,)),
            dma((sp_size,)), dma((sp_size,)),
            dma((4, sp_size, parts)), dma((members, 2, parts)),
            dma((4, parts)), dma((5,)),
        ],
        compiler_params=pltpu.CompilerParams(
            collective_id=0, has_side_effects=True, vmem_limit_bytes=60 * 1024 * 1024
        ),
    )(tokens, key_weight, value_weight, gate_rows)
    key_cache, value_cache = kv[:heads_here], kv[heads_here:]
    logit = logits.transpose(1, 0, 2).reshape(heads_here, sp_size * positions)
    log_gate = jax.nn.log_sigmoid(logit + forget_bias[:, None])
    cumulative = jnp.cumsum(log_gate, axis=1)
    query = lax.dynamic_index_in_dim(new_query, lax.axis_index("sp"), 0, keepdims=False)
    scores = (
        jnp.einsum("hd,hpd->hp", query, key_cache, preferred_element_type=jnp.float32) * scaling
        + cumulative[:, -1:] - cumulative
    )
    highest = jnp.max(scores, axis=1, keepdims=True)
    probs = jnp.exp(scores - highest)
    total = jnp.sum(probs, axis=1)
    attended = jnp.einsum("hp,hpd->hd", probs, value_cache.astype(jnp.float32)) / total[:, None]
    normed = attended * lax.rsqrt(jnp.mean(attended * attended, axis=-1, keepdims=True) + eps)
    return (
        key_cache[None], value_cache[None], cumulative[None], normed.astype(jnp.bfloat16)[None]
    )


def solution(mesh):
    in_specs = (
        P("gr", "sp", None),
        P(("gr", "sp"), "tp"),
        P(("gr", "sp"), "tp"),
        P(("gr", "sp"), "tp"),
        P("tp"),
        P("gr", "tp", None),
    )
    out_specs = (
        P(("gr", "sp"), "tp", None, None),
        P(("gr", "sp"), "tp", None, None),
        P(("gr", "sp"), "tp", None),
        P(("gr", "sp"), "tp", None),
    )
    return jax.shard_map(
        functools.partial(on_device, mesh.shape["gr"], mesh.shape["sp"]),
        mesh=mesh, in_specs=in_specs, out_specs=out_specs, check_vma=False,
    )
```

```python
import functools

import jax
import jax.numpy as jnp
from jax import lax
from jax.experimental import pallas as pl
from jax.experimental.pallas import tpu as pltpu
from jax.sharding import PartitionSpec as P

eps = 1e-06
MESH = pl.DeviceIdType.MESH


def exchange(
    gr_size, sp_size, tokens, key_weight, value_weight, gate_rows, kv_out, gate_out,
    tok, weights, full, gates, staged, gate_staged,
    tok_send, tok_recv, mate_send, mate_recv, w_send, w_recv, z_send, z_recv,
    gw_send, gw_recv, g_send, g_recv, o_send, o_recv, kept, local,
):
    g, s, t = lax.axis_index("gr"), lax.axis_index("sp"), lax.axis_index("tp")
    y, z = lax.rem(s, 2), s // 2
    levels = sp_size // 2
    sequences, positions, features = tokens.shape
    depth = weights.shape[1]
    parts, tile = full.shape[0], full.shape[2]
    width = parts * tile
    head_dim = kv_out.shape[2]
    heads = width // head_dim
    tile_heads = tile // head_dim
    members = gr_size * sp_size
    me = g * sp_size + s
    mate = t + 1 - 2 * lax.rem(t, 2)
    core = lax.rem(t, 2)
    quarter = sequences // 4

    gr_of = (g, 1 - g, g, 1 - g)
    y_of = (y, y, 1 - y, 1 - y)

    def where(r, level=None):
        return (gr_of[r], (z if level is None else level) * 2 + y_of[r], t)

    def remote(src, dst, send, recv, device):
        return pltpu.make_async_remote_copy(
            src_ref=src, dst_ref=dst, send_sem=send, recv_sem=recv,
            device_id=device, device_id_type=MESH,
        )

    taken = [
        pltpu.make_async_copy(ref, weights.at[k], local.at[k])
        for k, ref in enumerate((key_weight, value_weight))
    ]
    for copy in taken:
        copy.start()
    own_tokens = pltpu.make_async_copy(tokens, tok.at[0], local.at[2])
    own_tokens.start()
    own_gate = pltpu.make_async_copy(gate_rows, gates.at[me], local.at[3])
    own_gate.start()
    barrier = pltpu.get_barrier_semaphore()

    def greet(k, carry):
        @pl.when(k != me)
        def _():
            pl.semaphore_signal(
                barrier, inc=1, device_id=(k // sp_size, lax.rem(k, sp_size), t),
                device_id_type=MESH,
            )
        return carry

    lax.fori_loop(0, members, greet, 0)
    pl.semaphore_signal(barrier, inc=1, device_id=(g, s, mate), device_id_type=MESH)
    pl.semaphore_wait(barrier, members)

    def rows_at(r, level, c):
        return full.at[c, pl.ds(pl.multiple_of((gr_of[r] * sp_size + level * 2 + y_of[r]) * depth, depth), depth), :]

    def part_for(r, c):
        return weights.at[gr_of[r], :, pl.ds(pl.multiple_of(y_of[r] * width + c * tile, tile), tile)]

    def w_copy(r, c):
        return remote(part_for(r, c), rows_at(0, z, c), w_send.at[r, c], w_recv.at[r, c], where(r))

    def w_landing(r, c):
        return remote(part_for(r, c), rows_at(r, z, c), w_send.at[r, c], w_recv.at[r, c], where(r))

    def z_copy(direction, r, level, c, src=None):
        block = rows_at(r, level, c)
        to = z + 1 if direction == 0 else z - 1
        return remote(
            block if src is None else src, block, z_send.at[direction, level, r, c],
            z_recv.at[level, r, c], where(0, to),
        )

    def can_send(direction):
        return z < levels - 1 if direction == 0 else z > 0

    def pass_on(direction, r, level, c, src=None):
        @pl.when(can_send(direction))
        def _():
            z_copy(direction, r, level, c, src).start()

    def level_out(c):
        for direction in range(2):
            pass_on(direction, 0, z, c, part_for(0, c))
        for r in (1, 2, 3):
            w_landing(r, c).wait_recv()
            for direction in range(2):
                pass_on(direction, r, z, c)

    for copy in taken:
        copy.wait()
    for c in range(parts):
        for r in (3, 1, 2):
            w_copy(r, c).start()

    def gw_copy(k):
        return remote(
            gate_rows, gates.at[me], gw_send.at[k], gw_recv.at[me],
            (k // sp_size, lax.rem(k, sp_size), t),
        )

    def gw_landing(k):
        return remote(
            gate_rows, gates.at[k], gw_send.at[k], gw_recv.at[k],
            (k // sp_size, lax.rem(k, sp_size), t),
        )

    def others(fn):
        def turn(k, carry):
            @pl.when(k != me)
            def _():
                fn(k)
            return carry
        lax.fori_loop(0, members, turn, 0)

    others(lambda k: gw_copy(k).start())
    def piece(ref, half, c):
        return ref.at[pl.ds((half * 2 + c) * quarter, quarter)]

    def tok_copy(r, c):
        return remote(
            piece(tokens, core, c), piece(tok.at[r], core, c),
            tok_send.at[r, c], tok_recv.at[r, c], where(r),
        )

    def corner_copy(via, c):
        return remote(
            piece(tok.at[via], core, c), piece(tok.at[3], core, c),
            tok_send.at[3, c], tok_recv.at[3, c], where(3 - via),
        )

    def mate_copy(r, c, half):
        return remote(
            piece(tok.at[r], half, c), piece(tok.at[r], half, c),
            mate_send.at[r, c], mate_recv.at[r, c], (g, s, mate),
        )

    for c in range(2):
        tok_copy(1, c).start()
        tok_copy(2, 1 - c).start()

    def token_arrival(r, c):
        tok_copy(r, c).wait_recv()
        mate_copy(r, c, core).start()

    level_out(0)
    own_gate.wait()
    own_tokens.wait()

    others(lambda k: gw_landing(k).wait_recv())
    gate_full = jnp.concatenate([gates[k] for k in range(members)], axis=1).astype(jnp.bfloat16)

    def gate_copy(k):
        return remote(
            gate_staged.at[k], gate_out.at[s], g_send.at[k], g_recv.at[s], (g, k, t)
        )

    def gate_landing(k):
        return remote(
            gate_staged.at[k], gate_out.at[k], g_send.at[k], g_recv.at[k], (g, k, t)
        )

    def gate_turn(k, carry):
        gate_staged[k] = lax.dot_general(
            gate_full, tok[0, k], (((1,), (1,)), ((), ())),
            preferred_element_type=jnp.float32,
        )
        @pl.when(k != s)
        def _():
            gate_copy(k).start()
        @pl.when(k == s)
        def _():
            pltpu.make_async_copy(gate_staged.at[k], gate_out.at[k], local.at[4]).start()
        return carry

    lax.fori_loop(0, sequences, gate_turn, 0)

    def z_step(j, c):
        for r in range(4):
            @pl.when(z - j >= 0)
            def _():
                z_copy(0, r, z - j, c).wait_recv()
                pass_on(0, r, z - j, c)
            @pl.when(z + j < levels)
            def _():
                z_copy(1, r, z + j, c).wait_recv()
                pass_on(1, r, z + j, c)

    group = min(sequences, max(1, 512 // positions))
    groups = sequences // group

    def cache_at(their_g, their_y, their_z, b, c):
        return kv_out.at[
            pl.ds((their_g * 2 + their_y) * heads + c * tile_heads, tile_heads),
            pl.ds(pl.multiple_of((their_z * 2 + b) * positions, positions), positions),
            :,
        ]

    def out_copy(r, k, c):
        return remote(
            staged.at[r, c, :, k], cache_at(g, y, z, y_of[r], c),
            o_send.at[r, k, c], o_recv.at[me, y_of[r], c], (gr_of[r], k, t),
        )

    def out_landing(k, b, c):
        their_g, their_s = k // sp_size, lax.rem(k, sp_size)
        their_y, their_z = lax.rem(their_s, 2), their_s // 2
        return remote(
            staged.at[0, c, :, 0], cache_at(their_g, their_y, their_z, b, c),
            o_send.at[0, 0, c], o_recv.at[k, b, c], (their_g, their_s, t),
        )

    def keep_copy(r, c):
        return pltpu.make_async_copy(
            staged.at[r, c, :, s], cache_at(g, y, z, y_of[r], c), kept.at[r, c]
        )

    def products(r, c):
        def turn(m, carry):
            rows = tok[r, pl.ds(m * group, group)].reshape(group * positions, features)
            out = jnp.dot(rows, full[c], preferred_element_type=jnp.float32).astype(jnp.bfloat16)
            for h in range(tile_heads):
                staged[r, c, h, pl.ds(m * group, group)] = out[
                    :, h * head_dim : (h + 1) * head_dim
                ].reshape(group, positions, head_dim)
            return carry

        lax.fori_loop(0, groups, turn, 0)

        def send(i, carry):
            k = lax.rem(s + 1 + i, sp_size)
            if r in (1, 3):
                out_copy(r, k, c).start()
            else:
                @pl.when(k != s)
                def _():
                    out_copy(r, k, c).start()
                @pl.when(k == s)
                def _():
                    keep_copy(r, c).start()
            return carry

        lax.fori_loop(0, sequences, send, 0)

    def keep_rows(c):
        at = pl.multiple_of(me * depth, depth)
        columns = pl.ds(pl.multiple_of(y * width + c * tile, tile), tile)
        full[c, pl.ds(at, depth), :] = weights[g, :, columns]

    for c in range(parts):
        keep_rows(c)
    last = levels - 1
    for j in range(1, last):
        z_step(j, 0)
    for c in range(1, parts):
        level_out(c)
    token_arrival(1, 0)
    corner_copy(1, 0).start()
    token_arrival(2, 1)
    corner_copy(2, 1).start()
    z_step(last, 0)
    products(0, 0)
    for c in range(1, parts):
        z_step(1, c) if last > 1 else None
    token_arrival(1, 1)
    token_arrival(2, 0)
    for c in range(1, parts):
        for j in range(2, last):
            z_step(j, c)
    for r in (1, 2):
        for c in range(2):
            mate_copy(r, c, 1 - core).wait_recv()
        products(r, 0)
    for c in range(1, parts):
        z_step(last, c)
        for r in (0, 1):
            products(r, c)
    for c in range(2):
        token_arrival(3, c)
    for c in range(1, parts):
        products(2, c)
    for c in range(2):
        mate_copy(3, c, 1 - core).wait_recv()
    for c in range(parts):
        products(3, c)

    def landed(k):
        for b in range(2):
            for c in range(parts):
                out_landing(k, b, c).wait_recv()

    others(landed)
    for c in range(parts):
        keep_copy(0, c).wait()
        keep_copy(2, c).wait()

    def gate_landed(k, carry):
        @pl.when(k != s)
        def _():
            gate_landing(k).wait_recv()
            gate_copy(k).wait_send()
        @pl.when(k == s)
        def _():
            pltpu.make_async_copy(gate_staged.at[k], gate_out.at[k], local.at[4]).wait()
        return carry

    lax.fori_loop(0, sequences, gate_landed, 0)
    others(lambda k: gw_copy(k).wait_send())
    for r in (1, 2, 3):
        for c in range(parts):
            w_copy(r, c).wait_send()
        for c in range(2):
            mate_copy(r, c, core).wait_send()
    for c in range(2):
        tok_copy(1, c).wait_send()
        tok_copy(2, c).wait_send()
    corner_copy(1, 0).wait_send()
    corner_copy(2, 1).wait_send()
    for r in range(4):
        def sent(k, carry):
            for c in range(parts):
                if r in (1, 3):
                    out_copy(r, k, c).wait_send()
                else:
                    @pl.when(k != s)
                    def _():
                        out_copy(r, k, c).wait_send()
            return carry
        lax.fori_loop(0, sequences, sent, 0)
    for r in range(4):
        for c in range(parts):
            for direction in range(2):
                @pl.when(can_send(direction))
                def _():
                    z_copy(direction, r, z, c, part_for(0, c) if r == 0 else None).wait_send()
            for j in range(1, levels):
                @pl.when((z - j >= 0) & can_send(0))
                def _():
                    z_copy(0, r, z - j, c).wait_send()
                @pl.when((z + j < levels) & can_send(1))
                def _():
                    z_copy(1, r, z + j, c).wait_send()


def on_device(gr_size, sp_size, tokens, key_weight, value_weight, gate_weight, forget_bias, new_query):
    sequences, positions, features = tokens.shape
    heads_here = forget_bias.shape[0]
    head_dim = new_query.shape[2]
    scaling = head_dim ** (-0.5)
    members = gr_size * sp_size
    depth = key_weight.shape[0]
    width = 2 * key_weight.shape[1] // 4
    parts = 2 if width >= 2 * head_dim else 1
    tile = width // parts
    gate_rows = gate_weight.T.astype(jnp.float32)
    levels = sp_size // 2
    dma = pltpu.SemaphoreType.DMA
    kv, logits = pl.pallas_call(
        functools.partial(exchange, gr_size, sp_size),
        out_shape=(
            jax.ShapeDtypeStruct((2 * heads_here, sp_size * positions, head_dim), jnp.bfloat16),
            jax.ShapeDtypeStruct((sp_size, heads_here, positions), jnp.float32),
        ),
        in_specs=[pl.BlockSpec(memory_space=pl.ANY)] * 4,
        out_specs=(pl.BlockSpec(memory_space=pl.ANY),) * 2,
        scratch_shapes=[
            pltpu.VMEM((4, sequences, positions, features), jnp.bfloat16),
            pltpu.VMEM((2, depth, key_weight.shape[1]), jnp.bfloat16),
            pltpu.VMEM((parts, features, tile), jnp.bfloat16),
            pltpu.VMEM((members, heads_here, depth), jnp.float32),
            pltpu.VMEM((4, parts, tile // head_dim, sequences, positions, head_dim), jnp.bfloat16),
            pltpu.VMEM((sequences, heads_here, positions), jnp.float32),
            dma((4, 2)), dma((4, 2)), dma((4, 2)), dma((4, 2)),
            dma((4, parts)), dma((4, parts)),
            dma((2, levels, 4, parts)), dma((levels, 4, parts)),
            dma((members,)), dma((members,)),
            dma((sp_size,)), dma((sp_size,)),
            dma((4, sp_size, parts)), dma((members, 2, parts)),
            dma((4, parts)), dma((5,)),
        ],
        compiler_params=pltpu.CompilerParams(
            collective_id=0, has_side_effects=True, vmem_limit_bytes=60 * 1024 * 1024
        ),
    )(tokens, key_weight, value_weight, gate_rows)
    key_cache, value_cache = kv[:heads_here], kv[heads_here:]
    logit = logits.transpose(1, 0, 2).reshape(heads_here, sp_size * positions)
    log_gate = jax.nn.log_sigmoid(logit + forget_bias[:, None])
    cumulative = jnp.cumsum(log_gate, axis=1)
    query = lax.dynamic_index_in_dim(new_query, lax.axis_index("sp"), 0, keepdims=False)
    scores = (
        jnp.einsum("hd,hpd->hp", query, key_cache, preferred_element_type=jnp.float32) * scaling
        + cumulative[:, -1:] - cumulative
    )
    highest = jnp.max(scores, axis=1, keepdims=True)
    probs = jnp.exp(scores - highest)
    total = jnp.sum(probs, axis=1)
    attended = jnp.einsum("hp,hpd->hd", probs, value_cache.astype(jnp.float32)) / total[:, None]
    normed = attended * lax.rsqrt(jnp.mean(attended * attended, axis=-1, keepdims=True) + eps)
    return (
        key_cache[None], value_cache[None], cumulative[None], normed.astype(jnp.bfloat16)[None]
    )


def solution(mesh):
    in_specs = (
        P("gr", "sp", None),
        P(("gr", "sp"), "tp"),
        P(("gr", "sp"), "tp"),
        P(("gr", "sp"), "tp"),
        P("tp"),
        P("gr", "tp", None),
    )
    out_specs = (
        P(("gr", "sp"), "tp", None, None),
        P(("gr", "sp"), "tp", None, None),
        P(("gr", "sp"), "tp", None),
        P(("gr", "sp"), "tp", None),
    )
    return jax.shard_map(
        functools.partial(on_device, mesh.shape["gr"], mesh.shape["sp"]),
        mesh=mesh, in_specs=in_specs, out_specs=out_specs, check_vma=False,
    )
```
